256 devices in a mesh: fs: 32 (over z, y), tp: 8 (over x, core).
Axes of the slice: x: 4, y: 4, z: 8, core: 2. Of those that a mesh axis runs over, the one named last changes fastest.
Arguments:
- prompt: bfloat16 [32768, 2048], P(('fs', 'tp')), may hold values from -6 to 6
- norm_gain: float32 [2048], P('fs'), may hold values from 0.1 to 1.9
- up_trained: float32 [2048, 8192], P('fs', 'tp'), may hold values from -0.125 to 0.125
- down_trained: float32 [2048, 8192], P('fs', 'tp'), may hold values from -0.0625 to 0.0625
Outputs:
- up_served: bfloat16 [2048, 8192], P(None, 'tp')
- down_served: bfloat16 [8192, 2048], P('tp')
- mixed: bfloat16 [32768, 2048], P(('fs', 'tp'))
The draws below stay inside these ranges and needn't reach their ends.
All inputs are finite; a program needn't handle non-finite values.
Results may differ from the reference program's by a relative error of at most 0.014.
Values may be sent and summed in bfloat16 or wider, within the bound.
No kernel may reach another device: no remote copies, remote signals or barrier semaphores. Data moves between devices by JAX's collectives and lax.ppermute only.
A program may use at most 128 MiB of HBM per device.

```python
import jax
import jax.numpy as jnp
from jax import lax

D = 2048
FF = 8192
TOK_DEV = 128
TOKENS = 32768
N_FS = 32
N_TP = 8


def steps_of(rng, extent, split, least, high):
    def one(position, shards_of):
        steps = jax.random.uniform(jax.random.fold_in(jax.random.fold_in(rng, 6), position), (shards_of,), jnp.float32, least / len(split), high / len(split))
        return jnp.repeat(jnp.exp(steps), extent[position] // shards_of).reshape((-1,) + (1,) * (len(extent) - position - 1))

    loudness = one(*split[0])
    for cut in split[1:]:
        loudness = loudness * one(*cut)
    return loudness


def gaussian(stream_key, shape, deviation, reach, shards=(), kind=jnp.bfloat16):
    entries = jax.random.normal(stream_key, shape, jnp.float32) * deviation
    if len(shards) > 0:
        entries = steps_of(stream_key, shape, shards, -0.22, 0.18) * entries
    return jnp.clip(entries, min=-reach, max=reach).astype(kind)


def setup_inputs(seed: int = 0) -> dict:
    key_of = jax.random.split(jax.random.key(seed), 5)
    return {
        "prompt": gaussian(key_of[0], (TOKENS, D), 1.0, 6.0, ((0, 256),)),
        "norm_gain": jnp.clip(1.0 + 0.18 * jax.random.normal(key_of[1], (D,), jnp.float32), 0.1, 1.9),
        "up_trained": gaussian(key_of[2], (D, FF), D ** -0.5, 0.125, ((0, 32), (1, 8)), jnp.float32),
        "down_trained": gaussian(key_of[3], (D, FF), FF ** -0.5, 0.0625, ((0, 32), (1, 8)), jnp.float32),
    }


def reference(prompt, norm_gain, up_trained, down_trained):
    up_served = (norm_gain[:, None] * up_trained).astype(jnp.bfloat16)
    down_served = jnp.transpose(down_trained).astype(jnp.bfloat16)
    width = FF // N_TP
    groups = prompt.reshape(N_FS, N_TP * TOK_DEV, D)

    def one_group(rows):
        values = rows.astype(jnp.float32)
        scale = lax.rsqrt(lax.optimization_barrier(jnp.mean(values * values, axis=-1, keepdims=True)) + 1e-06)
        normed = (values * scale).astype(jnp.bfloat16)
        pre = jnp.dot(normed, up_served, preferred_element_type=jnp.float32)
        hidden = jnp.square(jax.nn.relu(pre)).astype(jnp.bfloat16)
        total = jnp.zeros((rows.shape[0], D), jnp.float32)
        for block in range(N_TP):
            partial_value = jnp.dot(hidden[:, block * width:(block + 1) * width], down_served[block * width:(block + 1) * width, :], preferred_element_type=jnp.float32).astype(jnp.bfloat16)
            total = total + partial_value.astype(jnp.float32)
        return total.astype(jnp.bfloat16)
    mixed = lax.map(one_group, groups).reshape(TOKENS, D)
    return (up_served, down_served, mixed)
```

```python
import functools

import jax
import jax.numpy as jnp
from jax import lax
from jax.experimental import pallas as pl
from jax.experimental.pallas import tpu as pltpu
from jax.sharding import PartitionSpec as P

NZ, NY, NX, NC = 8, 4, 4, 2


def rot(v, axis, n, by):
    return lax.ppermute(v, axis, [(i, (i + by) % n) for i in range(n)])


def norm_kernel(z_ref, x_ref, o_ref):
    x = x_ref[...].astype(jnp.float32)
    scale = lax.rsqrt(jnp.mean(x * x, axis=-1, keepdims=True) + 1e-06)
    width = x_ref.shape[1] // NZ
    for j in range(NZ):
        at = pl.multiple_of(lax.rem(z_ref[0] + j, NZ) * width, width)
        block = x_ref[:, pl.ds(at, width)].astype(jnp.float32)
        o_ref[:, j * width : (j + 1) * width] = (block * scale).astype(o_ref.dtype)


def normed_from(z, prompt):
    return pl.pallas_call(
        norm_kernel,
        out_shape=jax.ShapeDtypeStruct(prompt.shape, jnp.bfloat16),
        in_specs=[
            pl.BlockSpec(memory_space=pltpu.SMEM),
            pl.BlockSpec(memory_space=pltpu.VMEM),
        ],
        out_specs=pl.BlockSpec(memory_space=pltpu.VMEM),
        name="norm",
    )(z, prompt)


def by_y_kernel(y_ref, a_ref, b_ref, c_ref, d_ref, o_ref):
    for k, ref in enumerate((a_ref, b_ref, c_ref, d_ref)):
        o_ref[lax.rem(y_ref[0] + k, NY)] = ref[...]


def by_y(y, parts):
    rows, cols = parts[0].shape
    return pl.pallas_call(
        by_y_kernel,
        out_shape=jax.ShapeDtypeStruct((NY, rows, cols), parts[0].dtype),
        in_specs=[pl.BlockSpec(memory_space=pltpu.SMEM)]
        + [pl.BlockSpec(memory_space=pltpu.VMEM)] * NY,
        out_specs=pl.BlockSpec(memory_space=pltpu.VMEM),
        name="by_y",
    )(y, *parts).reshape(NY * rows, cols)


def place_kernel(spots, z_ref, *refs):
    sem, o_ref, parts = refs[-1], refs[-2], refs[:-2]
    copies = []
    for n, (part, (dz, off)) in enumerate(zip(parts, spots)):
        rows = part.shape[0]
        at = pl.multiple_of(lax.rem(z_ref[0] + dz + NZ, NZ) * 256 + off, rows)
        copies.append(pltpu.make_async_copy(part, o_ref.at[pl.ds(at, rows)], sem.at[n]))
        copies[-1].start()
    for c in copies:
        c.wait()


def place(z, parts, spots):
    return pl.pallas_call(
        functools.partial(place_kernel, spots),
        out_shape=jax.ShapeDtypeStruct((NZ * 256, parts[0].shape[1]), jnp.bfloat16),
        in_specs=[pl.BlockSpec(memory_space=pltpu.SMEM)]
        + [pl.BlockSpec(memory_space=pltpu.VMEM)] * len(parts),
        out_specs=pl.BlockSpec(memory_space=pl.ANY),
        scratch_shapes=[pltpu.SemaphoreType.DMA((len(parts),))],
        name="place",
    )(z, *parts)


def turn_kernel(dzs, first, zy_ref, *refs):
    if first:
        a_ref, b_ref, c_ref, d_ref, t_ref, o_ref, block, sem = refs
    else:
        a_ref, b_ref, c_ref, d_ref, _, t_ref, o_ref, block, sem = refs
    copies = []
    for j, dz in enumerate(dzs):
        for k, ref in enumerate((a_ref, b_ref, c_ref, d_ref)):
            block[lax.rem(zy_ref[1] + k, NY)] = ref[j * 64 : (j + 1) * 64, :]
        whole = block[...].reshape(256, block.shape[2])
        t_ref[:, j * 256 : (j + 1) * 256] = whole.T
        at = pl.multiple_of(lax.rem(zy_ref[0] + dz + NZ, NZ) * 256, 256)
        copies.append(
            pltpu.make_async_copy(
                t_ref.at[:, j * 256 : (j + 1) * 256], o_ref.at[:, pl.ds(at, 256)], sem.at[j]
            )
        )
    for c in copies:
        c.start()
    for c in copies:
        c.wait()


def turn(zy, parts, dzs, held=None):
    n, first = len(dzs), held is None
    cols = parts[0].shape[1]
    anywhere = pl.BlockSpec(memory_space=pl.ANY)
    vmem = pl.BlockSpec(memory_space=pltpu.VMEM)
    return pl.pallas_call(
        functools.partial(turn_kernel, dzs, first),
        out_shape=(
            jax.ShapeDtypeStruct((cols, n * 256), jnp.bfloat16),
            jax.ShapeDtypeStruct((cols, NZ * 256), jnp.bfloat16),
        ),
        in_specs=[pl.BlockSpec(memory_space=pltpu.SMEM)]
        + [vmem] * NY
        + ([] if first else [anywhere]),
        out_specs=(vmem, anywhere),
        scratch_shapes=[
            pltpu.VMEM((NY, 64, cols), jnp.bfloat16),
            pltpu.SemaphoreType.DMA((n,)),
        ],
        input_output_aliases={} if first else {5: 1},
        name="turn",
    )(zy, *parts, *(() if first else (held,)))


def total_kernel(z_ref, *refs):
    o_ref, ins = refs[-1], refs[:-1]
    for group in range(len(ins) // 4):
        a, b, c, d = ins[4 * group : 4 * group + 4]
        dzs = GROUPS[group]
        for j, dz in enumerate(dzs):
            cut = slice(j * 256, (j + 1) * 256)
            s = a[:, cut].astype(jnp.float32) + b[:, cut].astype(jnp.float32)
            s = s + (c[:, cut].astype(jnp.float32) + d[:, cut].astype(jnp.float32))
            at = pl.multiple_of(lax.rem(z_ref[0] + dz + NZ, NZ) * 256, 256)
            o_ref[:, pl.ds(at, 256)] = s.astype(o_ref.dtype)


def total(z, parts):
    return pl.pallas_call(
        total_kernel,
        out_shape=jax.ShapeDtypeStruct((parts[0].shape[0], NZ * 256), jnp.bfloat16),
        in_specs=[pl.BlockSpec(memory_space=pltpu.SMEM)]
        + [pl.BlockSpec(memory_space=pltpu.VMEM)] * len(parts),
        out_specs=pl.BlockSpec(memory_space=pltpu.VMEM),
        name="total",
    )(z, *parts)


GROUPS = ((0, 1, -1, 2, -2), (3, -3, 4))


def shards(prompt, norm_gain, up_trained, down_trained):
    z = lax.axis_index("z").astype(jnp.int32).reshape(1)
    y = lax.axis_index("y").astype(jnp.int32).reshape(1)
    zy = jnp.concatenate([z, y])
    up = (norm_gain[:, None] * up_trained).astype(jnp.bfloat16)
    down = down_trained.astype(jnp.bfloat16)

    up0 = by_y(y, (up, rot(up, "y", NY, -1), rot(up, "y", NY, 2), rot(up, "y", NY, 1)))

    normed = normed_from(z, prompt)
    mine = jnp.concatenate(
        [normed, rot(normed, "x", NX, -1), rot(normed, "x", NX, 2), rot(normed, "x", NX, 1)]
    )
    tokens = jnp.concatenate([mine, rot(mine, "c", NC, 1)])

    ups = {0: up0}
    downs = {0: down}
    for k in (1, 2, 3):
        ups[k] = rot(ups[k - 1], "z", NZ, -1)
        ups[-k] = rot(ups[1 - k], "z", NZ, 1)
        downs[k] = rot(downs[k - 1], "z", NZ, -1)
        downs[-k] = rot(downs[1 - k], "z", NZ, 1)
    far = (rot(ups[3][:128], "z", NZ, -1), rot(ups[-3][128:], "z", NZ, 1))
    downs[4] = rot(downs[3], "z", NZ, -1)

    turned, held = [], None
    for dzs in GROUPS:
        own = jnp.concatenate([downs[dz] for dz in dzs])
        parts = (own, rot(own, "y", NY, -1), rot(own, "y", NY, 2), rot(own, "y", NY, 1))
        t, held = turn(zy, parts, dzs, held)
        turned.append(t)

    order = (0, 1, -1, 2, -2, 3, -3)
    parts = [ups[dz] for dz in order] + list(far)
    up_served = place(z, parts, [(dz, 0) for dz in order] + [(4, 0), (4, 128)])

    def columns(dz):
        at = (dz % NZ) * 256
        return tokens[:, at : at + 256]

    near = GROUPS[0]
    acc = jnp.dot(
        jnp.concatenate([columns(dz) for dz in near], axis=1),
        jnp.concatenate([ups[dz] for dz in near]),
        preferred_element_type=jnp.float32,
    )
    pre = acc + jnp.dot(
        jnp.concatenate([columns(dz) for dz in (3, -3, 4)], axis=1),
        jnp.concatenate([ups[3], ups[-3], *far]),
        preferred_element_type=jnp.float32,
    )
    hidden = jnp.square(jax.nn.relu(pre)).astype(jnp.bfloat16)

    summed = []
    for t in turned:
        partial = jnp.dot(hidden, t, preferred_element_type=jnp.float32).astype(jnp.bfloat16)
        other = rot(partial[512:], "c", NC, 1)
        s = (partial[:512].astype(jnp.float32) + other.astype(jnp.float32)).astype(jnp.bfloat16)
        summed += [
            s[:128],
            rot(s[128:256], "x", NX, 1),
            rot(s[256:384], "x", NX, 2),
            rot(s[384:], "x", NX, -1),
        ]
    mixed = total(z, summed)
    return up_served, held, mixed


def solution(mesh):
    grid = jax.sharding.Mesh(mesh.devices.reshape(NZ, NY, NX, NC), ("z", "y", "x", "c"))
    fs, tp = ("z", "y"), ("x", "c")
    return jax.shard_map(
        shards,
        mesh=grid,
        in_specs=(P(fs + tp, None), P(fs), P(fs, tp), P(fs, tp)),
        out_specs=(P(None, tp), P(tp, None), P(fs + tp, None)),
        check_vma=False,
    )
```

```python
import functools

import jax
import jax.numpy as jnp
from jax import lax
from jax.experimental import pallas as pl
from jax.experimental.pallas import tpu as pltpu
from jax.sharding import PartitionSpec as P


NZ, NY, NX, NC = 8, 4, 4, 2
VMEM = pl.BlockSpec(memory_space=pltpu.VMEM)
ANY = pl.BlockSpec(memory_space=pl.ANY)
GROUPS = ((0, 1, -1, 2, -2), (3, -3, 4))
CHUNKS = ((0, 0, 2), (0, 2, 3), (1, 0, 3))
NEAR, MID = (-2, -1, 0, 1, 2), (-3, 3)


def rot(v, axis, n, by):
    return lax.ppermute(v, axis, [(i, (i + by) % n) for i in range(n)])


def limit(mib):
    return pltpu.CompilerParams(vmem_limit_bytes=mib * 2**20)


def cost(flops, nbytes):
    return pl.CostEstimate(flops=flops, bytes_accessed=nbytes, transcendentals=0)


def row_of(dz):
    return lax.rem(lax.axis_index("z") + (dz + NZ), NZ) * 256


def norm_kernel(x_ref, o_ref):
    x = x_ref[...].astype(jnp.float32)
    scale = lax.rsqrt(jnp.mean(x * x, axis=-1, keepdims=True) + 1e-06)
    for i in range(NZ):
        block = x_ref[:, pl.ds(pl.multiple_of(row_of(i - 3), 256), 256)].astype(jnp.float32)
        o_ref[:, i * 256 : (i + 1) * 256] = (block * scale).astype(o_ref.dtype)


def norm(x):
    return pl.pallas_call(
        norm_kernel,
        out_shape=jax.ShapeDtypeStruct(x.shape, jnp.bfloat16),
        in_specs=[VMEM],
        out_specs=VMEM,
        compiler_params=limit(8),
        name="norm",
    )(x)


def place_kernel(spots, cut, *refs):
    sem, o_ref, parts = refs[-1], refs[-2], refs[:-2]
    copies = []
    for n, (part, (spot, left)) in enumerate(zip(parts, spots)):
        rows = part.shape[0]
        at = pl.multiple_of(spot(), rows) if callable(spot) else spot
        wide = part.shape[1]
        if cut is not None:
            part, wide = part.at[:, cut[0] : cut[1]], cut[1] - cut[0]
        to = o_ref.at[pl.ds(at, rows), left : left + wide]
        copies.append(pltpu.make_async_copy(part, to, sem.at[n]))
        copies[-1].start()
    for c in copies:
        c.wait()


def place(parts, spots, shape, out, cut=None):
    return pl.pallas_call(
        functools.partial(place_kernel, spots, cut),
        out_shape=jax.ShapeDtypeStruct(shape, jnp.bfloat16),
        in_specs=[ANY] * len(parts),
        out_specs=out,
        scratch_shapes=[pltpu.SemaphoreType.DMA((len(parts),))],
        compiler_params=limit(8),
        name="place",
    )(*parts)


def up_kernel(n, more, last, *refs):
    own, oth, parts, o_ref = refs[:n], refs[n : 2 * n], refs[2 * n : 3 * n], refs[-1]
    half = own[0].shape[0]
    rhs = jnp.concatenate([p[...] for p in parts], axis=0)
    for c, group in enumerate((own, oth)):
        lhs = jnp.concatenate([t[...] for t in group], axis=1)
        dot = jnp.dot(lhs, rhs, preferred_element_type=jnp.float32)
        if more:
            dot = dot + refs[3 * n][c * half : (c + 1) * half, :]
        if last:
            dot = jnp.square(jnp.maximum(dot, 0.0))
        o_ref[c * half : (c + 1) * half, :] = dot.astype(o_ref.dtype)


def up_dot(own, oth, parts, acc=None, last=False):
    more, n = acc is not None, len(parts)
    rows, wide, tile = own.shape[0], parts[0][0].shape[1], 256
    tokens, pieces, depth = [], [], 0
    for p, at in parts:
        k = p.shape[0]
        tokens.append(pl.BlockSpec((rows, k), lambda j, i=at // k: (0, i)))
        pieces.append(pl.BlockSpec((k, tile), lambda j: (0, j)))
        depth += k
    col = pl.BlockSpec((2 * rows, tile), lambda j: (0, j))
    return pl.pallas_call(
        functools.partial(up_kernel, n, more, last),
        grid=(wide // tile,),
        out_shape=jax.ShapeDtypeStruct((2 * rows, wide), jnp.bfloat16 if last else jnp.float32),
        in_specs=tokens * 2 + pieces + ([col] if more else []),
        out_specs=col,
        compiler_params=limit(24),
        cost_estimate=cost(4 * rows * wide * depth, 6 * 2**20),
        name="up",
    )(*[own] * n, *[oth] * n, *[p for p, _ in parts], *((acc,) if more else ()))


def down_kernel(first, h_ref, a_ref, b_ref, c_ref, d_ref, own_ref, oth_ref):
    half = h_ref.shape[0] // 2
    rows = pl.ds(pl.multiple_of((pl.program_id(0) + first) * 64, 64), 64)
    rhs = jnp.concatenate([r[rows, :] for r in (a_ref, b_ref, c_ref, d_ref)], axis=0)
    for c, o_ref in enumerate((own_ref, oth_ref)):
        cut = slice(c * half, (c + 1) * half)
        o_ref[...] = lax.dot_general(
            h_ref[cut, :], rhs, (((1,), (1,)), ((), ())), preferred_element_type=jnp.float32
        ).astype(o_ref.dtype)


def down_dot(hidden, parts, first, n):
    rows, k = parts[0].shape
    m, wide = hidden.shape
    out = jax.ShapeDtypeStruct((m // 2, n * 256), jnp.bfloat16)
    col = pl.BlockSpec((m // 2, 256), lambda j: (0, j))
    return pl.pallas_call(
        functools.partial(down_kernel, first),
        grid=(n,),
        out_shape=(out, out),
        in_specs=[pl.BlockSpec((m, wide), lambda j: (0, 0))]
        + [pl.BlockSpec((rows, k), lambda j: (0, 0))] * NY,
        out_specs=(col, col),
        compiler_params=limit(24),
        cost_estimate=cost(2 * m * k * 256 * n, 6 * 2**20),
        name="down",
    )(hidden, *parts)


def turn_kernel(*refs):
    o_ref, block, out, sem = refs[-4:]
    y = lax.axis_index("y")

    def copy(seen):
        dz = jnp.where(lax.rem(seen, 2) == 1, (seen + 1) // 2, -(seen // 2))
        at = pl.multiple_of(row_of(dz), 256)
        return pltpu.make_async_copy(out.at[seen], o_ref.at[:, pl.ds(at, 256)], sem.at[seen])

    base = 0
    for g, dzs in enumerate(GROUPS):

        @pl.loop(0, len(dzs))
        def _(j, g=g, base=base):
            for k in range(NY):
                rows = pl.ds(pl.multiple_of(j * 64, 64), 64)
                block[lax.rem(y + k, NY)] = refs[4 * g + k][rows, :]
            out[base + j] = block[...].reshape(256, block.shape[2]).T
            copy(base + j).start()

        base += len(dzs)

    @pl.loop(0, NZ)
    def _(j):
        copy(j).wait()


def turn(parts):
    cols = parts[0].shape[1]
    return pl.pallas_call(
        turn_kernel,
        out_shape=jax.ShapeDtypeStruct((cols, NZ * 256), jnp.bfloat16),
        in_specs=[VMEM] * len(parts),
        out_specs=ANY,
        scratch_shapes=[
            pltpu.VMEM((NY, 64, cols), jnp.bfloat16),
            pltpu.VMEM((NZ, cols, 256), jnp.bfloat16),
            pltpu.SemaphoreType.DMA((NZ,)),
        ],
        compiler_params=limit(16),
        cost_estimate=cost(2 * 10**9, 8 * 2**20),
        name="turn",
    )(*parts)


def total_kernel(*refs):
    o_ref = refs[-1]
    shift = lax.axis_index("y") * 64
    for g, (at, first, n) in enumerate(CHUNKS):
        for j in range(n):
            cut = slice(j * 256, (j + 1) * 256)
            a, b, c, d = (r[:, cut].astype(jnp.float32) for r in refs[4 * g : 4 * g + 4])
            s = pltpu.roll((a + b) + (c + d), shift, 1)
            to = pl.ds(pl.multiple_of(row_of(GROUPS[at][first + j]), 256), 256)
            o_ref[:, to] = s.astype(o_ref.dtype)


def total(parts):
    return pl.pallas_call(
        total_kernel,
        out_shape=jax.ShapeDtypeStruct((parts[0].shape[0], NZ * 256), jnp.bfloat16),
        in_specs=[VMEM] * len(parts),
        out_specs=VMEM,
        compiler_params=limit(8),
        name="total",
    )(*parts)


def layer(prompt, norm_gain, up_trained, down_trained):
    up = (norm_gain[:, None] * up_trained).astype(jnp.bfloat16)
    down = down_trained.astype(jnp.bfloat16)

    def by_y(k):
        return lambda: lax.rem(lax.axis_index("y") + k, NY) * 64

    parts = (up, rot(up, "y", NY, -1), rot(up, "y", NY, 2), rot(up, "y", NY, 1))
    spots = [(by_y(k), 0) for k in range(NY)]
    wide = up.shape[1]
    ups = {0: place(parts, spots, (256, wide), VMEM)}

    normed = norm(prompt)
    parts = (normed, rot(normed, "x", NX, -1), rot(normed, "x", NX, 2), rot(normed, "x", NX, 1))
    own = place(parts, [(128 * k, 0) for k in range(NX)], (512, NZ * 256), VMEM)
    oth = rot(own, "c", NC, 1)

    downs = {0: down}
    for k in (1, 2, 3):
        ups[k] = rot(ups[k - 1], "z", NZ, -1)
        ups[-k] = rot(ups[1 - k], "z", NZ, 1)
        frm, hops = (0, k) if k < 3 else (2, 1)
        downs[k] = rot(downs[frm], "z", NZ, -hops)
        downs[-k] = rot(downs[-frm], "z", NZ, hops)
    far = (rot(ups[3][:128], "z", NZ, -1), rot(ups[-3][128:], "z", NZ, 1))
    downs[4] = rot(downs[3], "z", NZ, -1)

    parted = []
    for dzs in GROUPS:
        mine = jnp.concatenate([downs[dz] for dz in dzs])
        parted.append((mine, rot(mine, "y", NY, -1), rot(mine, "y", NY, 2), rot(mine, "y", NY, 1)))

    acc = up_dot(own, oth, [(ups[dz], (dz + 3) * 256) for dz in NEAR])
    acc = up_dot(own, oth, [(ups[dz], (dz + 3) * 256) for dz in MID], acc)
    hidden = up_dot(own, oth, [(far[0], 7 * 256), (far[1], 7 * 256 + 128)], acc, last=True)

    summed = []
    for at, first, n in CHUNKS:
        mine, theirs = down_dot(hidden, parted[at], first, n)
        got = rot(theirs, "c", NC, 1)
        s = (mine.astype(jnp.float32) + got.astype(jnp.float32)).astype(jnp.bfloat16)
        summed += [
            s[:128],
            rot(s[128:256], "x", NX, 1),
            rot(s[256:384], "x", NX, 2),
            rot(s[384:], "x", NX, -1),
        ]
    mixed = total(summed)
    down_served = turn([p for parts in parted for p in parts])
    parts = [ups[dz] for dz in NEAR + MID] + list(far)
    spots = [(functools.partial(row_of, dz), 0) for dz in NEAR + MID]
    spots += [(functools.partial(row_of, 4), 0), (lambda: row_of(4) + 128, 0)]
    up_served = place(parts, spots, (NZ * 256, wide), ANY)
    return up_served, down_served, mixed


def solution(mesh):
    grid = jax.sharding.Mesh(mesh.devices.reshape(NZ, NY, NX, NC), ("z", "y", "x", "c"))
    fs, tp = ("z", "y"), ("x", "c")
    return jax.shard_map(
        layer,
        mesh=grid,
        in_specs=(P(fs + tp, None), P(fs), P(fs, tp), P(fs, tp)),
        out_specs=(P(None, tp), P(tp, None), P(fs + tp, None)),
        check_vma=False,
    )
```

```python
import functools

import jax
import jax.numpy as jnp
from jax import lax
from jax.experimental import pallas as pl
from jax.experimental.pallas import tpu as pltpu
from jax.sharding import PartitionSpec as P


NZ, NY, NX, NC = 8, 4, 4, 2
VMEM = pl.BlockSpec(memory_space=pltpu.VMEM)
ANY = pl.BlockSpec(memory_space=pl.ANY)
GROUPS = ((0, 1, -1, 2, -2), (3, -3, 4))
CHUNKS = ((0, 0, 2), (0, 2, 3), (1, 0, 3))
NEAR, MID = (-2, -1, 0, 1, 2), (-3, 3)


def rot(v, axis, n, by):
    return lax.ppermute(v, axis, [(i, (i + by) % n) for i in range(n)])


def limit(mib):
    return pltpu.CompilerParams(vmem_limit_bytes=mib * 2**20)


def cost(flops, nbytes):
    return pl.CostEstimate(flops=flops, bytes_accessed=nbytes, transcendentals=0)


def row_of(dz):
    return lax.rem(lax.axis_index("z") + (dz + NZ), NZ) * 256


def norm_kernel(x_ref, o_ref):
    x = x_ref[...].astype(jnp.float32)
    scale = lax.rsqrt(jnp.mean(x * x, axis=-1, keepdims=True) + 1e-06)
    for i in range(NZ):
        block = x_ref[:, pl.ds(pl.multiple_of(row_of(i - 3), 256), 256)].astype(jnp.float32)
        o_ref[:, i * 256 : (i + 1) * 256] = (block * scale).astype(o_ref.dtype)


def norm(x):
    return pl.pallas_call(
        norm_kernel,
        out_shape=jax.ShapeDtypeStruct(x.shape, jnp.bfloat16),
        in_specs=[VMEM],
        out_specs=VMEM,
        compiler_params=limit(8),
        name="norm",
    )(x)


def place_kernel(spots, cut, *refs):
    sem, o_ref, parts = refs[-1], refs[-2], refs[:-2]
    copies = []
    for n, (part, (spot, left)) in enumerate(zip(parts, spots)):
        rows = part.shape[0]
        at = pl.multiple_of(spot(), rows) if callable(spot) else spot
        wide = part.shape[1]
        if cut is not None:
            part, wide = part.at[:, cut[0] : cut[1]], cut[1] - cut[0]
        to = o_ref.at[pl.ds(at, rows), left : left + wide]
        copies.append(pltpu.make_async_copy(part, to, sem.at[n]))
        copies[-1].start()
    for c in copies:
        c.wait()


def place(parts, spots, shape, out, cut=None):
    return pl.pallas_call(
        functools.partial(place_kernel, spots, cut),
        out_shape=jax.ShapeDtypeStruct(shape, jnp.bfloat16),
        in_specs=[ANY] * len(parts),
        out_specs=out,
        scratch_shapes=[pltpu.SemaphoreType.DMA((len(parts),))],
        compiler_params=limit(8),
        name="place",
    )(*parts)


def up_kernel(places, more, last, *refs):
    n, o_ref = len(places), refs[-1]
    parts = refs[2 : 2 + n]
    half, tile = refs[0].shape[0], 256

    @pl.loop(0, o_ref.shape[1] // tile)
    def _(j):
        cols = pl.ds(pl.multiple_of(j * tile, tile), tile)
        rhs = jnp.concatenate([p[:, cols] for p in parts], axis=0)
        for c in range(2):
            rows = slice(c * half, (c + 1) * half)
            lhs = [refs[c][:, at : at + p.shape[0]] for p, at in zip(parts, places)]
            lhs = jnp.concatenate(lhs, axis=1)
            dot = jnp.dot(lhs, rhs, preferred_element_type=jnp.float32)
            if more:
                dot = dot + refs[2 + n][rows, cols]
            if last:
                dot = jnp.square(jnp.maximum(dot, 0.0))
            o_ref[rows, cols] = dot.astype(o_ref.dtype)


def up_dot(own, oth, parts, acc=None, last=False):
    rows, wide = 2 * own.shape[0], parts[0][0].shape[1]
    depth = sum(p.shape[0] for p, _ in parts)
    ins = (own, oth, *[p for p, _ in parts]) + (() if acc is None else (acc,))
    places = tuple(at for _, at in parts)
    return pl.pallas_call(
        functools.partial(up_kernel, places, acc is not None, last),
        out_shape=jax.ShapeDtypeStruct((rows, wide), jnp.bfloat16 if last else jnp.float32),
        in_specs=[VMEM] * len(ins),
        out_specs=VMEM,
        compiler_params=limit(24),
        cost_estimate=cost(2 * rows * wide * depth, 6 * 2**20),
        name="up",
    )(*ins)


def down_kernel(first, h_ref, a_ref, b_ref, c_ref, d_ref, own_ref, oth_ref):
    half = h_ref.shape[0] // 2

    @pl.loop(0, own_ref.shape[1] // 256)
    def _(j):
        rows = pl.ds(pl.multiple_of((j + first) * 64, 64), 64)
        cols = pl.ds(pl.multiple_of(j * 256, 256), 256)
        rhs = jnp.concatenate([r[rows, :] for r in (a_ref, b_ref, c_ref, d_ref)], axis=0)
        for c, o_ref in enumerate((own_ref, oth_ref)):
            cut = slice(c * half, (c + 1) * half)
            o_ref[:, cols] = lax.dot_general(
                h_ref[cut, :], rhs, (((1,), (1,)), ((), ())), preferred_element_type=jnp.float32
            ).astype(o_ref.dtype)


def down_dot(hidden, parts, first, n):
    m, k = hidden.shape
    out = jax.ShapeDtypeStruct((m // 2, n * 256), jnp.bfloat16)
    return pl.pallas_call(
        functools.partial(down_kernel, first),
        out_shape=(out, out),
        in_specs=[VMEM] * (1 + NY),
        out_specs=(VMEM, VMEM),
        compiler_params=limit(24),
        cost_estimate=cost(2 * m * k * 256 * n, 6 * 2**20),
        name="down",
    )(hidden, *parts)


def turn_kernel(*refs):
    o_ref, block, out, sem = refs[-4:]
    y = lax.axis_index("y")

    def copy(seen):
        dz = jnp.where(lax.rem(seen, 2) == 1, (seen + 1) // 2, -(seen // 2))
        at = pl.multiple_of(row_of(dz), 256)
        return pltpu.make_async_copy(out.at[seen], o_ref.at[:, pl.ds(at, 256)], sem.at[seen])

    base = 0
    for g, dzs in enumerate(GROUPS):

        @pl.loop(0, len(dzs))
        def _(j, g=g, base=base):
            for k in range(NY):
                rows = pl.ds(pl.multiple_of(j * 64, 64), 64)
                block[lax.rem(y + k, NY)] = refs[4 * g + k][rows, :]
            out[base + j] = block[...].reshape(256, block.shape[2]).T
            copy(base + j).start()

        base += len(dzs)

    @pl.loop(0, NZ)
    def _(j):
        copy(j).wait()


def turn(parts):
    cols = parts[0].shape[1]
    return pl.pallas_call(
        turn_kernel,
        out_shape=jax.ShapeDtypeStruct((cols, NZ * 256), jnp.bfloat16),
        in_specs=[VMEM] * len(parts),
        out_specs=ANY,
        scratch_shapes=[
            pltpu.VMEM((NY, 64, cols), jnp.bfloat16),
            pltpu.VMEM((NZ, cols, 256), jnp.bfloat16),
            pltpu.SemaphoreType.DMA((NZ,)),
        ],
        compiler_params=limit(16),
        cost_estimate=cost(2 * 10**9, 8 * 2**20),
        name="turn",
    )(*parts)


def total_kernel(*refs):
    o_ref = refs[-1]
    shift = lax.axis_index("y") * 64
    for g, (at, first, n) in enumerate(CHUNKS):
        for j in range(n):
            cut = slice(j * 256, (j + 1) * 256)
            a, b, c, d = (r[:, cut].astype(jnp.float32) for r in refs[4 * g : 4 * g + 4])
            s = pltpu.roll((a + b) + (c + d), shift, 1)
            to = pl.ds(pl.multiple_of(row_of(GROUPS[at][first + j]), 256), 256)
            o_ref[:, to] = s.astype(o_ref.dtype)


def total(parts):
    return pl.pallas_call(
        total_kernel,
        out_shape=jax.ShapeDtypeStruct((parts[0].shape[0], NZ * 256), jnp.bfloat16),
        in_specs=[VMEM] * len(parts),
        out_specs=VMEM,
        compiler_params=limit(8),
        name="total",
    )(*parts)


def layer(prompt, norm_gain, up_trained, down_trained):
    up = (norm_gain[:, None] * up_trained).astype(jnp.bfloat16)
    down = down_trained.astype(jnp.bfloat16)

    def by_y(k):
        return lambda: lax.rem(lax.axis_index("y") + k, NY) * 64

    parts = (up, rot(up, "y", NY, -1), rot(up, "y", NY, 2), rot(up, "y", NY, 1))
    spots = [(by_y(k), 0) for k in range(NY)]
    wide = up.shape[1]
    ups = {0: place(parts, spots, (256, wide), VMEM)}

    normed = norm(prompt)
    parts = (normed, rot(normed, "x", NX, -1), rot(normed, "x", NX, 2), rot(normed, "x", NX, 1))
    own = place(parts, [(128 * k, 0) for k in range(NX)], (512, NZ * 256), VMEM)
    oth = rot(own, "c", NC, 1)

    downs = {0: down}
    for k in (1, 2, 3):
        ups[k] = rot(ups[k - 1], "z", NZ, -1)
        ups[-k] = rot(ups[1 - k], "z", NZ, 1)
        frm, hops = (0, k) if k < 3 else (2, 1)
        downs[k] = rot(downs[frm], "z", NZ, -hops)
        downs[-k] = rot(downs[-frm], "z", NZ, hops)
    far = (rot(ups[3][:128], "z", NZ, -1), rot(ups[-3][128:], "z", NZ, 1))
    downs[4] = rot(downs[3], "z", NZ, -1)

    parted = []
    for dzs in GROUPS:
        mine = jnp.concatenate([downs[dz] for dz in dzs])
        parted.append((mine, rot(mine, "y", NY, -1), rot(mine, "y", NY, 2), rot(mine, "y", NY, 1)))

    acc = up_dot(own, oth, [(ups[dz], (dz + 3) * 256) for dz in NEAR])
    acc = up_dot(own, oth, [(ups[dz], (dz + 3) * 256) for dz in MID], acc)
    hidden = up_dot(own, oth, [(far[0], 7 * 256), (far[1], 7 * 256 + 128)], acc, last=True)

    summed = []
    for at, first, n in CHUNKS:
        mine, theirs = down_dot(hidden, parted[at], first, n)
        got = rot(theirs, "c", NC, 1)
        s = (mine.astype(jnp.float32) + got.astype(jnp.float32)).astype(jnp.bfloat16)
        summed += [
            s[:128],
            rot(s[128:256], "x", NX, 1),
            rot(s[256:384], "x", NX, 2),
            rot(s[384:], "x", NX, -1),
        ]
    mixed = total(summed)
    down_served = turn([p for parts in parted for p in parts])
    parts = [ups[dz] for dz in NEAR + MID] + list(far)
    spots = [(functools.partial(row_of, dz), 0) for dz in NEAR + MID]
    spots += [(functools.partial(row_of, 4), 0), (lambda: row_of(4) + 128, 0)]
    up_served = place(parts, spots, (NZ * 256, wide), ANY)
    return up_served, down_served, mixed


def solution(mesh):
    grid = jax.sharding.Mesh(mesh.devices.reshape(NZ, NY, NX, NC), ("z", "y", "x", "c"))
    fs, tp = ("z", "y"), ("x", "c")
    return jax.shard_map(
        layer,
        mesh=grid,
        in_specs=(P(fs + tp, None), P(fs), P(fs, tp), P(fs, tp)),
        out_specs=(P(None, tp), P(tp, None), P(fs + tp, None)),
        check_vma=False,
    )
```
